32 devices in a mesh: ep: 32 (over z, y, x, core).
Axes of the slice: x: 2, y: 2, z: 4, core: 2. Of those that a mesh axis runs over, the one named last changes fastest.
Arguments:
- tokens: bfloat16 [512, 2048], P('ep'), may hold values from -6 to 6
- state: float32 [2, 512, 2048], P(None, 'ep'), may hold values from -4 to 4
- norm_mix: float32 [2048], replicated, may hold values from 0.1 to 1.9
- w_drive: bfloat16 [2048, 512], replicated, may hold values from -0.125 to 0.125
- lam_real: float32 [32, 64], replicated, may hold values from -1 to -0.05
- lam_imag: float32 [32, 64], replicated, may hold values from -3 to 3
- log_step: float32 [32], replicated, may hold values from -2.5 to 0.5
- b_real: float32 [32, 64, 16], replicated, may hold values from -1 to 1
- b_imag: float32 [32, 64, 16], replicated, may hold values from -1 to 1
- readout_real: float32 [32, 16, 64], replicated, may hold values from -0.5 to 0.5
- readout_imaginary: float32 [32, 16, 64], replicated, may hold values from -0.5 to 0.5
- d_skip: float32 [512], replicated, may hold values from -4 to 4
- w_value: bfloat16 [512, 512], replicated, may hold values from -0.25 to 0.25
- w_glugate: bfloat16 [512, 512], replicated, may hold values from -0.25 to 0.25
- w_output: bfloat16 [512, 2048], replicated, may hold values from -0.25 to 0.25
- norm_ffn: float32 [2048], replicated, may hold values from 0.1 to 1.9
- w_group: bfloat16 [2048, 4], replicated, may hold values from -0.125 to 0.125
- w_expert: bfloat16 [2048, 32], replicated, may hold values from -0.125 to 0.125
- route_ids: int32 [512, 6], P('ep'), may hold values from 0 to 31, all different within a row; in each aligned block of 16 rows (0 to 15, 16 to 31, ...) at most 7 rows name the same one
- expert_gate: bfloat16 [32, 2048, 512], P('ep'), may hold values from -0.125 to 0.125
- expert_up: bfloat16 [32, 2048, 512], P('ep'), may hold values from -0.125 to 0.125
- expert_down: bfloat16 [32, 512, 2048], P('ep'), may hold values from -1 to 1
- dense_vector: float32 [2048], replicated, may hold values from -0.125 to 0.125
- dense_gate: bfloat16 [2048, 8192], P(None, 'ep'), may hold values from -0.125 to 0.125
- dense_up: bfloat16 [2048, 8192], P(None, 'ep'), may hold values from -0.125 to 0.125
- dense_down: bfloat16 [8192, 2048], P('ep'), may hold values from -0.25 to 0.25
Outputs:
- layer_out: bfloat16 [512, 2048], P('ep')
- new_state: float32 [2, 512, 2048], P(None, 'ep')
The draws below stay inside these ranges and needn't reach their ends.
Inputs may be any that keep to these rules, and one draw needn't show every extreme that they name: `route_ids`: each row names 6 different experts. Among the rows of one device no expert is named more than 7 times, a bound that some block reaches.
All inputs are finite; a program needn't handle non-finite values.
Results may differ from the reference program's by a relative error of at most 0.018.
Values may be sent and summed in bfloat16 or wider, within the bound.
A program may use at most 128 MiB of HBM per device.

```python
import math
import jax
import jax.numpy as jnp
import numpy as np
from jax import lax

D = 2048
S5W = 512
CH = 16
P_SIZE = 64
G = 32
GP = 2048
DENSE_FF = 8192
EXP_FF = 512
GROUPS = 4
TOPK = 6
SEQ_DEV = 16
SEQS = 512
EXPERTS = 32
CAP = 7
N_EP = 32


def steps_of(stream_key, extent, cuts, smallest, largest):
    level, own = 1.0, jax.random.fold_in(stream_key, 6)
    for position, shards_of in cuts:
        steps = jnp.exp(jax.random.uniform(jax.random.fold_in(own, position), (shards_of,), jnp.float32, smallest / len(cuts), largest / len(cuts)))
        level = level * jnp.repeat(steps, extent[position] // shards_of).reshape([-1 if axis == position else 1 for axis in range(len(extent))])
    return level


def assign_block(stream_key, own, number, rows, amount, top, limit, slope):
    ranking = jax.random.permutation(stream_key, amount)
    crowded, usual = load_shares(amount, rows * top, limit, slope, True), load_shares(amount, rows * top, limit, slope, False)
    places = jnp.arange(amount)

    def named(tallies, rotation):
        used = int((tallies > 0).sum())
        fixed = max(1, used // 4)
        moved = fixed + (places - fixed + rotation * (used - fixed)) % max(1, amount - fixed)
        return jnp.zeros((amount,), jnp.int32).at[ranking[jnp.where(places < fixed, places, moved)]].set(jnp.asarray(tallies, jnp.int32))

    tallies = jnp.where(number % 4 == 0, named(crowded, number // 4), named(usual, number - number // 4 - 1))
    mixed = jax.random.permutation(jax.random.fold_in(own, 3), amount)
    source_of, sink = mixed[0:amount // 2 * 2:2], mixed[1:amount // 2 * 2:2]
    margin = jnp.minimum(tallies[source_of] - 1, limit - tallies[sink]) // 2
    margin = jnp.where((source_of == ranking[0]) | (sink == ranking[0]) | (tallies[sink] == 0), 0, jnp.maximum(margin, 0))
    moved = jax.random.randint(jax.random.fold_in(own, 4), (amount // 2,), 0, 1 << 20) % (margin + 1)
    tallies = tallies.at[source_of].add(-moved).at[sink].add(moved)
    items = jnp.searchsorted(jnp.cumsum(tallies), jnp.arange(rows * top), side="right").astype(jnp.int32)
    listing = items.reshape(top, rows).T
    listing = listing[jax.random.permutation(jax.random.fold_in(own, 1), rows)]
    rotation = jax.random.randint(jax.random.fold_in(own, 2), (rows, 1), 0, top)
    return jnp.take_along_axis(listing, (jnp.arange(top)[None, :] + rotation) % top, axis=1)


def load_shares(number_of, total, most, skew, full):
    loads = [(1 << 20) // math.isqrt(grade ** skew) + 1 for grade in range(1, number_of + 1)]
    largest = most if full else min(most, max(-(-total // number_of), total * loads[0] // sum(loads)))
    least = 1 if total - largest >= number_of - 1 else 0
    holding, rest = [largest] + [least] * (number_of - 1), total - largest - least * (number_of - 1)
    while rest > 0:
        free = [i for i in range(1, number_of) if holding[i] < largest] or [i for i in range(1, number_of) if holding[i] < most]
        pool, remaining = sum([loads[i] for i in free]), rest
        for i in free:
            addition = min(most - holding[i], max(1, remaining * loads[i] // pool), rest)
            holding[i] = holding[i] + addition
            rest = rest - addition
    return np.array(holding)


def bell_draw(stream_key, extent, spread, limit, cuts=(), kind=jnp.bfloat16):
    array = spread * jax.random.normal(stream_key, extent, jnp.float32)
    if cuts:
        array = array * steps_of(stream_key, extent, cuts, -0.22, 0.18)
    return jnp.clip(array, -limit, limit).astype(kind)


def setup_inputs(seed: int = 0) -> dict:
    key_list = jax.random.split(jax.random.key(seed), 27)
    tokens = bell_draw(key_list[0], (SEQS, D), 1.0, 6.0, ((0, 32),))
    state = bell_draw(key_list[1], (2, SEQS, GP), 0.5, 4.0, ((1, 32),), jnp.float32)
    norm_mix = jnp.clip(1.0 + 0.18 * jax.random.normal(key_list[2], (D,), jnp.float32), 0.1, 1.9)
    w_drive = bell_draw(key_list[3], (D, S5W), D ** -0.5, 0.125)
    lam_real = jnp.clip(jax.random.uniform(key_list[4], (G, P_SIZE), jnp.float32, -1.0, -0.05), -1.0, -0.05)
    lam_imag = jnp.clip(jax.random.uniform(key_list[5], (G, P_SIZE), jnp.float32, -3.0, 3.0), -3.0, 3.0)
    log_step = jnp.clip(jax.random.uniform(key_list[6], (G,), jnp.float32, -2.5, 0.5), -2.5, 0.5)
    b_real = bell_draw(key_list[7], (G, P_SIZE, CH), (2 * CH) ** -0.5, 1.0, (), jnp.float32)
    b_imag = bell_draw(key_list[8], (G, P_SIZE, CH), (2 * CH) ** -0.5, 1.0, (), jnp.float32)
    readout_real = bell_draw(key_list[9], (G, CH, P_SIZE), (2 * P_SIZE) ** -0.5, 0.5, (), jnp.float32)
    readout_imaginary = bell_draw(key_list[10], (G, CH, P_SIZE), (2 * P_SIZE) ** -0.5, 0.5, (), jnp.float32)
    d_skip = bell_draw(key_list[11], (S5W,), 1.0, 4.0, (), jnp.float32)
    w_value = bell_draw(key_list[12], (S5W, S5W), S5W ** -0.5, 0.25)
    w_glugate = bell_draw(key_list[13], (S5W, S5W), S5W ** -0.5, 0.25)
    w_output = bell_draw(key_list[14], (S5W, D), S5W ** -0.5, 0.25)
    norm_ffn = jnp.clip(1.0 + 0.18 * jax.random.normal(key_list[15], (D,), jnp.float32), 0.1, 1.9)
    w_group = bell_draw(key_list[16], (D, GROUPS), D ** -0.5, 0.125)
    w_expert = bell_draw(key_list[17], (D, EXPERTS), D ** -0.5, 0.125)
    route_ids_keys = jax.random.split(jax.random.fold_in(key_list[18], 1), SEQS // SEQ_DEV)
    route_ids_turns = jax.random.permutation(jax.random.fold_in(key_list[18], 3), SEQS // SEQ_DEV)
    route_ids = jax.vmap(lambda own, number: assign_block(jax.random.fold_in(key_list[18], 2), own, number, SEQ_DEV, EXPERTS, TOPK, CAP, 2))(route_ids_keys, route_ids_turns).reshape((SEQS, TOPK))
    expert_gate = bell_draw(key_list[19], (EXPERTS, D, EXP_FF), D ** -0.5, 0.125, ((0, 32),))
    expert_up = bell_draw(key_list[20], (EXPERTS, D, EXP_FF), D ** -0.5, 0.125, ((0, 32),))
    expert_down = bell_draw(key_list[21], (EXPERTS, EXP_FF, D), (EXP_FF // 16) ** -0.5, 1.0, ((0, 32),))
    dense_vector = bell_draw(key_list[22], (D,), D ** -0.5, 0.125, (), jnp.float32)
    dense_gate = bell_draw(key_list[23], (D, DENSE_FF), D ** -0.5, 0.125, ((1, 32),))
    dense_up = bell_draw(key_list[24], (D, DENSE_FF), D ** -0.5, 0.125, ((1, 32),))
    dense_down = bell_draw(key_list[25], (DENSE_FF, D), (DENSE_FF // 16) ** -0.5, 0.25, ((0, 32),))
    return dict(tokens=tokens, state=state, norm_mix=norm_mix, w_drive=w_drive, lam_real=lam_real, lam_imag=lam_imag, log_step=log_step, b_real=b_real, b_imag=b_imag, readout_real=readout_real, readout_imaginary=readout_imaginary, d_skip=d_skip, w_value=w_value, w_glugate=w_glugate, w_output=w_output, norm_ffn=norm_ffn, w_group=w_group, w_expert=w_expert, route_ids=route_ids, expert_gate=expert_gate, expert_up=expert_up, expert_down=expert_down, dense_vector=dense_vector, dense_gate=dense_gate, dense_up=dense_up, dense_down=dense_down)


EPS = 1e-05
HIGH_PRECISION = lax.Precision.HIGHEST

def rms_scale(values, gain):
    widened = values.astype(jnp.float32)
    scaled = widened * lax.rsqrt(lax.optimization_barrier(jnp.mean(widened * widened, axis=-1, keepdims=True)) + EPS)
    return (scaled * gain).astype(jnp.bfloat16)

def state_mixer(tokens, state, norm_mix, w_drive, lam_real, lam_imag, log_step, b_real, b_imag, readout_real, readout_imaginary, d_skip, w_value, w_glugate, w_output):
    row_count = tokens.shape[0]
    group_count, state_dimension = lam_real.shape
    channels = b_real.shape[2]
    normed_in = rms_scale(tokens, norm_mix)
    drive = jnp.dot(normed_in, w_drive, preferred_element_type=jnp.float32).astype(jnp.bfloat16)
    time_step = jnp.exp(log_step)[:, None]
    magnitude = jnp.exp(lam_real * time_step)
    decay_re = magnitude * jnp.cos(lam_imag * time_step)
    decay_im = magnitude * jnp.sin(lam_imag * time_step)
    modulus = lam_real * lam_real + lam_imag * lam_imag
    factor_re = ((decay_re - 1.0) * lam_real + decay_im * lam_imag) / modulus
    factor_im = (decay_im * lam_real - (decay_re - 1.0) * lam_imag) / modulus
    map_re = factor_re[:, :, None] * b_real - factor_im[:, :, None] * b_imag
    map_im = factor_re[:, :, None] * b_imag + factor_im[:, :, None] * b_real
    drive_wide = drive.astype(jnp.float32)
    grouped = drive_wide.reshape(row_count, group_count, channels)
    input_re = jnp.einsum('gpc,sgc->sgp', map_re, grouped, precision=HIGH_PRECISION)
    input_im = jnp.einsum('gpc,sgc->sgp', map_im, grouped, precision=HIGH_PRECISION)
    old_re = state[0].reshape(row_count, group_count, state_dimension)
    old_im = state[1].reshape(row_count, group_count, state_dimension)
    incoming_real = decay_re * old_re - decay_im * old_im + input_re
    incoming_imaginary = decay_re * old_im + decay_im * old_re + input_im
    projected_output = jnp.einsum('xej,fxj->fxe', readout_real, incoming_real, precision=HIGH_PRECISION) - jnp.einsum('xej,fxj->fxe', readout_imaginary, incoming_imaginary, precision=HIGH_PRECISION)
    readout = jax.nn.gelu(projected_output.reshape(row_count, group_count * channels) + d_skip * drive_wide).astype(jnp.bfloat16)
    value_part = jnp.dot(readout, w_value, preferred_element_type=jnp.float32)
    gate_part = jnp.dot(readout, w_glugate, preferred_element_type=jnp.float32)
    mixed = (value_part * jax.nn.sigmoid(gate_part)).astype(jnp.bfloat16)
    resid = (tokens.astype(jnp.float32) + jnp.dot(mixed, w_output, preferred_element_type=jnp.float32)).astype(jnp.bfloat16)
    new_state = jnp.stack([incoming_real.reshape(row_count, -1), incoming_imaginary.reshape(row_count, -1)])
    return (resid, new_state)

def route_gates(normed, w_group, w_expert, route_ids):
    row_count = normed.shape[0]
    group_count = w_group.shape[1]
    expert_count = w_expert.shape[1]
    per_group = expert_count // group_count
    group_exp = jnp.exp(jnp.dot(normed, w_group, preferred_element_type=jnp.float32))
    group_prob = group_exp / lax.optimization_barrier(jnp.sum(group_exp, axis=1, keepdims=True))
    inner_exp = jnp.exp(jnp.dot(normed, w_expert, preferred_element_type=jnp.float32)).reshape(row_count, group_count, per_group)
    inner_prob = inner_exp / lax.optimization_barrier(jnp.sum(inner_exp, axis=2, keepdims=True))
    joint = (group_prob[:, :, None] * inner_prob).reshape(row_count, expert_count)
    inner_flat = inner_prob.reshape(row_count, expert_count)
    matched = route_ids[:, :, None] == jnp.arange(expert_count, dtype=jnp.int32)[None, None, :]
    picked_joint = lax.optimization_barrier(jnp.sum(jnp.where(matched, joint[:, None, :], 0.0), axis=2))
    picked_inner = lax.optimization_barrier(jnp.sum(jnp.where(matched, inner_flat[:, None, :], 0.0), axis=2))
    return picked_joint / lax.optimization_barrier(jnp.sum(picked_inner, axis=1, keepdims=True))

def expert_rows(rows_in, w_gate, w_up, w_down):
    gate_part = jnp.dot(rows_in, w_gate, preferred_element_type=jnp.float32)
    up_part = jnp.dot(rows_in, w_up, preferred_element_type=jnp.float32)
    hidden = (jax.nn.silu(gate_part) * up_part).astype(jnp.bfloat16)
    return jnp.dot(hidden, w_down, preferred_element_type=jnp.float32).astype(jnp.bfloat16)

def reference(tokens, state, norm_mix, w_drive, lam_real, lam_imag, log_step, b_real, b_imag, readout_real, readout_imaginary, d_skip, w_value, w_glugate, w_output, norm_ffn, w_group, w_expert, route_ids, expert_gate, expert_up, expert_down, dense_vector, dense_gate, dense_up, dense_down):
    resid, new_state = state_mixer(tokens, state, norm_mix, w_drive, lam_real, lam_imag, log_step, b_real, b_imag, readout_real, readout_imaginary, d_skip, w_value, w_glugate, w_output)
    normed = rms_scale(resid, norm_ffn)
    gates = route_gates(normed, w_group, w_expert, route_ids)
    total_rows, width = normed.shape
    expert_count = w_expert.shape[1]
    slot_total = N_EP * CAP
    positions = jnp.arange(total_rows, dtype=jnp.int32)

    def visit(carry, matmul_argument):
        expert_id, w_gate, w_up, w_down = matmul_argument
        matched = route_ids == expert_id
        weight = lax.optimization_barrier(jnp.sum(jnp.where(matched, gates, 0.0), axis=1))
        chosen = jnp.any(matched, axis=1)
        ordinal = jnp.cumsum(chosen.astype(jnp.int32)) - 1
        target = jnp.where(chosen, ordinal, slot_total).astype(jnp.int32)
        slot_token = jnp.zeros((slot_total,), jnp.int32).at[target].set(positions, mode='drop')
        slot_live = jnp.zeros((slot_total,), jnp.float32).at[target].set(1.0, mode='drop')
        result = expert_rows(normed[slot_token], w_gate, w_up, w_down)
        contrib = result.astype(jnp.float32) * (weight[slot_token] * slot_live)[:, None]
        return (carry.at[slot_token].add(contrib), None)
    start_sum = jnp.zeros((total_rows, width), jnp.float32)
    expert_ids = jnp.arange(expert_count, dtype=jnp.int32)
    expert_sum, _ = lax.scan(visit, start_sum, (expert_ids, expert_gate, expert_up, expert_down))
    normed_wide = normed.astype(jnp.float32)
    branch_gate = jax.nn.sigmoid(jnp.dot(normed_wide, dense_vector, precision=HIGH_PRECISION))
    dense_g = jnp.dot(normed, dense_gate, preferred_element_type=jnp.float32)
    dense_u = jnp.dot(normed, dense_up, preferred_element_type=jnp.float32)
    dense_hidden = (branch_gate[:, None] * jax.nn.silu(dense_g) * dense_u).astype(jnp.bfloat16)
    dense_sum = jnp.dot(dense_hidden, dense_down, preferred_element_type=jnp.float32)
    layer_out = (resid.astype(jnp.float32) + dense_sum + expert_sum).astype(jnp.bfloat16)
    return (layer_out, new_state)
```

```python
import functools

import jax
import jax.numpy as jnp
from jax import lax
from jax.experimental import pallas as pl
from jax.experimental.pallas import tpu as pltpu
from jax.sharding import PartitionSpec as P

EPS = 1e-05
HIGH_PRECISION = lax.Precision.HIGHEST


def rms_scale(values, gain):
    widened = values.astype(jnp.float32)
    scaled = widened * lax.rsqrt(jnp.mean(widened * widened, axis=-1, keepdims=True) + EPS)
    return (scaled * gain).astype(jnp.bfloat16)


def state_mixer(
    tokens,
    state,
    norm_mix,
    w_drive,
    lam_real,
    lam_imag,
    log_step,
    b_real,
    b_imag,
    readout_real,
    readout_imaginary,
    d_skip,
    w_value,
    w_glugate,
    w_output,
):
    row_count = tokens.shape[0]
    group_count, state_dimension = lam_real.shape
    channels = b_real.shape[2]
    normed_in = rms_scale(tokens, norm_mix)
    drive = jnp.dot(normed_in, w_drive, preferred_element_type=jnp.float32).astype(jnp.bfloat16)
    time_step = jnp.exp(log_step)[:, None]
    magnitude = jnp.exp(lam_real * time_step)
    decay_re = magnitude * jnp.cos(lam_imag * time_step)
    decay_im = magnitude * jnp.sin(lam_imag * time_step)
    modulus = lam_real * lam_real + lam_imag * lam_imag
    factor_re = ((decay_re - 1.0) * lam_real + decay_im * lam_imag) / modulus
    factor_im = (decay_im * lam_real - (decay_re - 1.0) * lam_imag) / modulus
    map_re = factor_re[:, :, None] * b_real - factor_im[:, :, None] * b_imag
    map_im = factor_re[:, :, None] * b_imag + factor_im[:, :, None] * b_real
    drive_wide = drive.astype(jnp.float32)
    grouped = drive_wide.reshape(row_count, group_count, channels)
    input_re = jnp.einsum("gpc,sgc->sgp", map_re, grouped, precision=HIGH_PRECISION)
    input_im = jnp.einsum("gpc,sgc->sgp", map_im, grouped, precision=HIGH_PRECISION)
    old_re = state[0].reshape(row_count, group_count, state_dimension)
    old_im = state[1].reshape(row_count, group_count, state_dimension)
    incoming_real = decay_re * old_re - decay_im * old_im + input_re
    incoming_imaginary = decay_re * old_im + decay_im * old_re + input_im
    projected_output = jnp.einsum(
        "xej,fxj->fxe", readout_real, incoming_real, precision=HIGH_PRECISION
    ) - jnp.einsum("xej,fxj->fxe", readout_imaginary, incoming_imaginary, precision=HIGH_PRECISION)
    readout = jax.nn.gelu(
        projected_output.reshape(row_count, group_count * channels) + d_skip * drive_wide
    ).astype(jnp.bfloat16)
    value_part = jnp.dot(readout, w_value, preferred_element_type=jnp.float32)
    gate_part = jnp.dot(readout, w_glugate, preferred_element_type=jnp.float32)
    mixed = (value_part * jax.nn.sigmoid(gate_part)).astype(jnp.bfloat16)
    resid = (
        tokens.astype(jnp.float32) + jnp.dot(mixed, w_output, preferred_element_type=jnp.float32)
    ).astype(jnp.bfloat16)
    new_state = jnp.stack(
        [incoming_real.reshape(row_count, -1), incoming_imaginary.reshape(row_count, -1)]
    )
    return (resid, new_state)


def route_gates(normed, w_group, w_expert, route_ids):
    row_count = normed.shape[0]
    group_count = w_group.shape[1]
    expert_count = w_expert.shape[1]
    per_group = expert_count // group_count
    group_exp = jnp.exp(jnp.dot(normed, w_group, preferred_element_type=jnp.float32))
    group_prob = group_exp / jnp.sum(group_exp, axis=1, keepdims=True)
    inner_exp = jnp.exp(jnp.dot(normed, w_expert, preferred_element_type=jnp.float32)).reshape(
        row_count, group_count, per_group
    )
    inner_prob = inner_exp / jnp.sum(inner_exp, axis=2, keepdims=True)
    joint = (group_prob[:, :, None] * inner_prob).reshape(row_count, expert_count)
    inner_flat = inner_prob.reshape(row_count, expert_count)
    matched = jnp.any(
        route_ids[:, :, None] == jnp.arange(expert_count, dtype=jnp.int32)[None, None, :], axis=1
    )
    chosen_inner = jnp.sum(jnp.where(matched, inner_flat, 0.0), axis=1, keepdims=True)
    return jnp.where(matched, joint / chosen_inner, 0.0)


MESH_ID = pl.DeviceIdType.MESH


def chip_offsets(chips):
    far = chips // 4
    steps = [(f, m, n) for f in range(far) for m in range(2) for n in range(2)]
    return sorted(steps, key=lambda s: (min(s[0], far - s[0]) + s[1] + s[2], s))[1:]


def chip_at(chip, step, chips, sign):
    far = chips // 4
    f, m, n = step
    return (
        ((chip // 4 + far + sign * f) % far) * 4
        + ((chip // 2 + m) % 2) * 2
        + (chip + n) % 2
    )


def meet(partners):
    barrier = pltpu.get_barrier_semaphore()
    for partner in partners:
        pl.semaphore_signal(barrier, inc=1, device_id=(partner,), device_id_type=MESH_ID)
    pl.semaphore_wait(barrier, len(partners))


def remote(src, dst, send_sem, recv_sem, device):
    return pltpu.make_async_remote_copy(
        src_ref=src,
        dst_ref=dst,
        send_sem=send_sem,
        recv_sem=recv_sem,
        device_id=(device,),
        device_id_type=MESH_ID,
    )


def gather_kernel(chips, own_ref, all_ref, own_sem, send_sem, recv_sem, pass_send, pass_recv):
    me = lax.axis_index("ep")
    chip, core = me // 2, me % 2
    sibling = chip * 2 + 1 - core
    steps = chip_offsets(chips)
    targets = [chip_at(chip, step, chips, 1) * 2 + core for step in steps]
    meet([sibling] + targets)
    stay = pltpu.make_async_copy(own_ref, all_ref.at[me], own_sem)
    sends = [
        remote(own_ref, all_ref.at[me], send_sem.at[i], recv_sem.at[i], target)
        for i, target in enumerate(targets)
    ]
    for send in sends:
        send.start()
    passes = [remote(own_ref, all_ref.at[me], pass_send.at[0], pass_recv.at[0], sibling)]
    passes[0].start()
    stay.start()
    for i, step in enumerate(steps):
        source = chip_at(chip, step, chips, -1) * 2 + core
        sends[i].wait_recv()
        onward = remote(
            all_ref.at[source],
            all_ref.at[source],
            pass_send.at[i + 1],
            pass_recv.at[i + 1],
            sibling,
        )
        onward.start()
        passes.append(onward)
    stay.wait()
    for send in sends:
        send.wait_send()
    for onward in passes:
        onward.wait()


def gather_rows(own, n):
    chips = n // 2
    rows, width = own.shape
    return pl.pallas_call(
        functools.partial(gather_kernel, chips),
        out_shape=jax.ShapeDtypeStruct((n, rows, width), own.dtype),
        in_specs=[pl.BlockSpec(memory_space=pltpu.VMEM)],
        out_specs=pl.BlockSpec(memory_space=pltpu.VMEM),
        scratch_shapes=[
            pltpu.SemaphoreType.DMA,
            pltpu.SemaphoreType.DMA((chips - 1,)),
            pltpu.SemaphoreType.DMA((chips - 1,)),
            pltpu.SemaphoreType.DMA((chips,)),
            pltpu.SemaphoreType.DMA((chips,)),
        ],
        compiler_params=pltpu.CompilerParams(collective_id=0, has_side_effects=True),
        cost_estimate=pl.CostEstimate(flops=0, bytes_accessed=60_000_000, transcendentals=0),
        name="gather_rows",
    )(own)


def scatter_kernel(
    chips,
    terms_ref,
    resid_ref,
    out_ref,
    pair_in,
    staged,
    landed,
    total,
    pair_send,
    pair_recv,
    send_sem,
    recv_sem,
):
    me = lax.axis_index("ep")
    chip, core = me // 2, me % 2
    sibling = chip * 2 + 1 - core
    steps = chip_offsets(chips)[::-1]
    others = [chip_at(chip, step, chips, 1) for step in steps]
    meet([sibling] + [other * 2 + core for other in others])
    pairs = []
    for i, other in enumerate(others + [chip]):
        pair = remote(
            terms_ref.at[other * 2 + 1 - core],
            pair_in.at[i],
            pair_send.at[i],
            pair_recv.at[i],
            sibling,
        )
        pair.start()
        pairs.append(pair)
    sends = []
    for i, other in enumerate(others):
        pairs[i].wait_recv()
        mine = terms_ref[other * 2 + core].astype(jnp.float32)
        staged[i] = (mine + pair_in[i].astype(jnp.float32)).astype(staged.dtype)
        sends.append(
            remote(staged.at[i], landed.at[i], send_sem.at[i], recv_sem.at[i], other * 2 + core)
        )
        if i:
            sends[i - 1].start()
    last = len(others)
    pairs[last].wait_recv()
    total[...] = (
        resid_ref[...].astype(jnp.float32)
        + terms_ref[me].astype(jnp.float32)
        + pair_in[last].astype(jnp.float32)
    )
    sends[-1].start()
    for i in range(len(others))[::-1]:
        sends[i].wait_recv()
        total[...] += landed[i].astype(jnp.float32)
    out_ref[...] = total[...].astype(out_ref.dtype)
    for send in sends:
        send.wait_send()
    for pair in pairs:
        pair.wait_send()


def scatter_rows(terms, resid):
    n, rows, width = terms.shape
    chips = n // 2
    return pl.pallas_call(
        functools.partial(scatter_kernel, chips),
        out_shape=jax.ShapeDtypeStruct(resid.shape, resid.dtype),
        in_specs=[pl.BlockSpec(memory_space=pltpu.VMEM)] * 2,
        out_specs=pl.BlockSpec(memory_space=pltpu.VMEM),
        scratch_shapes=[
            pltpu.VMEM((chips, rows, width), terms.dtype),
            pltpu.VMEM((chips - 1, rows, width), terms.dtype),
            pltpu.VMEM((chips - 1, rows, width), terms.dtype),
            pltpu.VMEM((rows, width), jnp.float32),
            pltpu.SemaphoreType.DMA((chips,)),
            pltpu.SemaphoreType.DMA((chips,)),
            pltpu.SemaphoreType.DMA((chips - 1,)),
            pltpu.SemaphoreType.DMA((chips - 1,)),
        ],
        compiler_params=pltpu.CompilerParams(collective_id=1, has_side_effects=True),
        name="scatter_rows",
    )(terms, resid)


def in_pieces(values):
    high = lax.reduce_precision(values, 8, 7)
    middle = lax.reduce_precision(values - high, 8, 7)
    return jnp.concatenate([high, middle, values - high - middle], axis=1).astype(jnp.bfloat16)


def on_device(
    n,
    tokens,
    state,
    norm_mix,
    w_drive,
    lam_real,
    lam_imag,
    log_step,
    b_real,
    b_imag,
    readout_real,
    readout_imaginary,
    d_skip,
    w_value,
    w_glugate,
    w_output,
    norm_ffn,
    w_group,
    w_expert,
    route_ids,
    expert_gate,
    expert_up,
    expert_down,
    dense_vector,
    dense_gate,
    dense_up,
    dense_down,
):
    resid, new_state = state_mixer(
        tokens,
        state,
        norm_mix,
        w_drive,
        lam_real,
        lam_imag,
        log_step,
        b_real,
        b_imag,
        readout_real,
        readout_imaginary,
        d_skip,
        w_value,
        w_glugate,
        w_output,
    )
    normed = rms_scale(resid, norm_ffn)
    expert_count = w_expert.shape[1]
    rows, width = normed.shape
    gates = route_gates(normed, w_group, w_expert, route_ids)
    branch_gate = jax.nn.sigmoid(
        jnp.dot(normed.astype(jnp.float32), dense_vector, precision=HIGH_PRECISION)
    )
    scales = in_pieces(jnp.concatenate([gates, branch_gate[:, None]], axis=1))
    scales = jnp.pad(scales, ((0, 0), (0, -scales.shape[1] % 128)))
    gathered = gather_rows(jnp.concatenate([normed, scales], axis=1), n)
    gathered = gathered.reshape(n * rows, -1)
    piece, scales = gathered[:, :width], gathered[:, width:].astype(jnp.float32)
    stride = expert_count + 1
    column = jnp.arange(scales.shape[1], dtype=jnp.int32)
    owner = jnp.where(column < 3 * stride, column % stride, stride)
    me = lax.axis_index("ep")
    own_weight = jnp.sum(jnp.where(owner == me, scales, 0.0), axis=1, keepdims=True)
    branch_all = jnp.sum(jnp.where(owner == expert_count, scales, 0.0), axis=1, keepdims=True)

    def hidden_units(w_gate, w_up, scale):
        gate_part = jnp.dot(piece, w_gate, preferred_element_type=jnp.float32)
        up_part = jnp.dot(piece, w_up, preferred_element_type=jnp.float32)
        return (scale * jax.nn.silu(gate_part) * up_part).astype(jnp.bfloat16)

    dense_hidden = hidden_units(dense_gate, dense_up, branch_all)
    expert_hidden = hidden_units(expert_gate[0], expert_up[0], own_weight)
    terms = jnp.dot(dense_hidden, dense_down, preferred_element_type=jnp.float32) + jnp.dot(
        expert_hidden, expert_down[0], preferred_element_type=jnp.float32
    )
    layer_out = scatter_rows(terms.astype(jnp.bfloat16).reshape(n, rows, width), resid)
    return (layer_out, new_state)


def solution(mesh):
    placed = (
        P("ep", None),
        P(None, "ep", None),
        P(),
        P(),
        P(),
        P(),
        P(),
        P(),
        P(),
        P(),
        P(),
        P(),
        P(),
        P(),
        P(),
        P(),
        P(),
        P(),
        P("ep", None),
        P("ep", None, None),
        P("ep", None, None),
        P("ep", None, None),
        P(),
        P(None, "ep"),
        P(None, "ep"),
        P("ep", None),
    )
    return jax.shard_map(
        functools.partial(on_device, mesh.shape["ep"]),
        mesh=mesh,
        in_specs=placed,
        out_specs=(P("ep", None), P(None, "ep", None)),
        check_vma=False,
    )
```

```python
import functools

import jax
import jax.numpy as jnp
from jax import lax
from jax.experimental import pallas as pl
from jax.experimental.pallas import tpu as pltpu
from jax.sharding import PartitionSpec as P

EPS = 1e-05
HIGH_PRECISION = lax.Precision.HIGHEST


def rms_scale(values, gain):
    widened = values.astype(jnp.float32)
    scaled = widened * lax.rsqrt(jnp.mean(widened * widened, axis=-1, keepdims=True) + EPS)
    return (scaled * gain).astype(jnp.bfloat16)


def state_mixer(
    tokens,
    state,
    norm_mix,
    w_drive,
    lam_real,
    lam_imag,
    log_step,
    b_real,
    b_imag,
    readout_real,
    readout_imaginary,
    d_skip,
    w_value,
    w_glugate,
    w_output,
):
    row_count = tokens.shape[0]
    group_count, state_dimension = lam_real.shape
    channels = b_real.shape[2]
    normed_in = rms_scale(tokens, norm_mix)
    drive = jnp.dot(normed_in, w_drive, preferred_element_type=jnp.float32).astype(jnp.bfloat16)
    time_step = jnp.exp(log_step)[:, None]
    magnitude = jnp.exp(lam_real * time_step)
    decay_re = magnitude * jnp.cos(lam_imag * time_step)
    decay_im = magnitude * jnp.sin(lam_imag * time_step)
    modulus = lam_real * lam_real + lam_imag * lam_imag
    factor_re = ((decay_re - 1.0) * lam_real + decay_im * lam_imag) / modulus
    factor_im = (decay_im * lam_real - (decay_re - 1.0) * lam_imag) / modulus
    map_re = factor_re[:, :, None] * b_real - factor_im[:, :, None] * b_imag
    map_im = factor_re[:, :, None] * b_imag + factor_im[:, :, None] * b_real
    drive_wide = drive.astype(jnp.float32)
    grouped = drive_wide.reshape(row_count, group_count, channels)
    input_re = jnp.einsum("gpc,sgc->sgp", map_re, grouped, precision=HIGH_PRECISION)
    input_im = jnp.einsum("gpc,sgc->sgp", map_im, grouped, precision=HIGH_PRECISION)
    old_re = state[0].reshape(row_count, group_count, state_dimension)
    old_im = state[1].reshape(row_count, group_count, state_dimension)
    incoming_real = decay_re * old_re - decay_im * old_im + input_re
    incoming_imaginary = decay_re * old_im + decay_im * old_re + input_im
    projected_output = jnp.einsum(
        "xej,fxj->fxe", readout_real, incoming_real, precision=HIGH_PRECISION
    ) - jnp.einsum("xej,fxj->fxe", readout_imaginary, incoming_imaginary, precision=HIGH_PRECISION)
    readout = jax.nn.gelu(
        projected_output.reshape(row_count, group_count * channels) + d_skip * drive_wide
    ).astype(jnp.bfloat16)
    value_part = jnp.dot(readout, w_value, preferred_element_type=jnp.float32)
    gate_part = jnp.dot(readout, w_glugate, preferred_element_type=jnp.float32)
    mixed = (value_part * jax.nn.sigmoid(gate_part)).astype(jnp.bfloat16)
    resid = (
        tokens.astype(jnp.float32) + jnp.dot(mixed, w_output, preferred_element_type=jnp.float32)
    ).astype(jnp.bfloat16)
    new_state = jnp.stack(
        [incoming_real.reshape(row_count, -1), incoming_imaginary.reshape(row_count, -1)]
    )
    return (resid, new_state)


def route_gates(normed, w_group, w_expert, route_ids):
    row_count = normed.shape[0]
    group_count = w_group.shape[1]
    expert_count = w_expert.shape[1]
    per_group = expert_count // group_count
    group_exp = jnp.exp(jnp.dot(normed, w_group, preferred_element_type=jnp.float32))
    group_prob = group_exp / jnp.sum(group_exp, axis=1, keepdims=True)
    inner_exp = jnp.exp(jnp.dot(normed, w_expert, preferred_element_type=jnp.float32)).reshape(
        row_count, group_count, per_group
    )
    inner_prob = inner_exp / jnp.sum(inner_exp, axis=2, keepdims=True)
    joint = (group_prob[:, :, None] * inner_prob).reshape(row_count, expert_count)
    inner_flat = inner_prob.reshape(row_count, expert_count)
    matched = jnp.any(
        route_ids[:, :, None] == jnp.arange(expert_count, dtype=jnp.int32)[None, None, :], axis=1
    )
    chosen_inner = jnp.sum(jnp.where(matched, inner_flat, 0.0), axis=1, keepdims=True)
    return jnp.where(matched, joint / chosen_inner, 0.0)


MESH_ID = pl.DeviceIdType.MESH


class Place:
    def __init__(self, chips):
        me = lax.axis_index("ep")
        chip, core = me // 2, me % 2
        near, middle = 1 - 2 * (chip % 2), 2 - 4 * ((chip // 2) % 2)
        self.me, self.chip, self.core = me, chip, core
        self.far, self.line = chips // 4, chip // 4
        self.sibling = chip * 2 + 1 - core
        first = chip + (1 - core) * near + core * middle
        second = chip + core * near + (1 - core) * middle
        self.first, self.second = first * 2 + core, second * 2 + core
        self.own_row, self.first_row, self.second_row = chip % 4, first % 4, second % 4
        self.across_row = 3 - self.own_row

    def chip_of(self, step, row):
        return ((self.line + self.far + step) % self.far) * 4 + row

    def block(self, step, row):
        return self.chip_of(step, row) * 2 + self.core

    def partners(self):
        line = [self.block(step, self.own_row) for step in range(1, self.far)]
        return [self.sibling, self.first, self.second] + line


def meet(partners):
    barrier = pltpu.get_barrier_semaphore()
    for partner in partners:
        pl.semaphore_signal(barrier, inc=1, device_id=(partner,), device_id_type=MESH_ID)
    pl.semaphore_wait(barrier, len(partners))


def remote(src, dst, send_sem, recv_sem, device):
    return pltpu.make_async_remote_copy(
        src_ref=src,
        dst_ref=dst,
        send_sem=send_sem,
        recv_sem=recv_sem,
        device_id=(device,),
        device_id_type=MESH_ID,
    )


def gather_kernel(
    chips,
    own_ref,
    all_ref,
    own_sem,
    line_send,
    line_recv,
    first_send,
    first_recv,
    second_send,
    second_recv,
    pass_send,
    pass_recv,
):
    at = Place(chips)
    far = at.far
    meet(at.partners())
    started = []

    def send(block, send_sem, recv_sem, slot, device):
        source = own_ref if block is None else all_ref.at[block]
        target = all_ref.at[at.me if block is None else block]
        copy = remote(source, target, send_sem.at[slot], recv_sem.at[slot], device)
        copy.start()
        started.append(copy)
        return copy

    lines = [
        send(None, line_send, line_recv, step - 1, at.block(step, at.own_row))
        for step in range(1, far)
    ]
    firsts, seconds, passes = [], [], []
    stay = pltpu.make_async_copy(own_ref, all_ref.at[at.me], own_sem)
    for step in range(far + 1):
        if step < far:
            if step:
                lines[step - 1].wait_recv()
            block = at.block(-step, at.own_row) if step else None
            firsts.append(send(block, first_send, first_recv, step, at.first))
            seconds.append(send(block, second_send, second_recv, step, at.second))
            passes.append(send(block, pass_send, pass_recv, step, at.sibling))
            if step == 0:
                stay.start()
        if step:
            firsts[step - 1].wait_recv()
            block = at.block(1 - step, at.first_row)
            slot = far + step - 1
            seconds.append(send(block, second_send, second_recv, slot, at.second))
            passes.append(send(block, pass_send, pass_recv, slot, at.sibling))
    arriving = [(step, at.second_row) for step in range(far)]
    arriving += [(step, at.across_row) for step in range(far)]
    by_slot = {}
    order = list(range(far)) + [far + step for step in range(far)]
    sent_order = []
    for step in range(far + 1):
        if step < far:
            sent_order.append(step)
        if step:
            sent_order.append(far + step - 1)
    for slot, copy in zip(sent_order, seconds):
        by_slot[slot] = copy
    for slot in order:
        step, row = arriving[slot]
        by_slot[slot].wait_recv()
        block = at.block(-step, row)
        passes.append(send(block, pass_send, pass_recv, 2 * far + slot, at.sibling))
    stay.wait()
    for copy in passes:
        copy.wait_recv()
    for copy in started:
        copy.wait_send()


def gather_rows(own, n):
    chips = n // 2
    rows, width = own.shape
    return pl.pallas_call(
        functools.partial(gather_kernel, chips),
        out_shape=jax.ShapeDtypeStruct((n, rows, width), own.dtype),
        in_specs=[pl.BlockSpec(memory_space=pltpu.VMEM)],
        out_specs=pl.BlockSpec(memory_space=pltpu.VMEM),
        scratch_shapes=[
            pltpu.SemaphoreType.DMA,
            pltpu.SemaphoreType.DMA((chips // 4 - 1,)),
            pltpu.SemaphoreType.DMA((chips // 4 - 1,)),
            pltpu.SemaphoreType.DMA((chips // 4,)),
            pltpu.SemaphoreType.DMA((chips // 4,)),
            pltpu.SemaphoreType.DMA((chips // 2,)),
            pltpu.SemaphoreType.DMA((chips // 2,)),
            pltpu.SemaphoreType.DMA((chips,)),
            pltpu.SemaphoreType.DMA((chips,)),
        ],
        compiler_params=pltpu.CompilerParams(collective_id=0, has_side_effects=True),
        cost_estimate=pl.CostEstimate(flops=0, bytes_accessed=60_000_000, transcendentals=0),
        name="gather_rows",
    )(own)


def scatter_kernel(
    chips,
    terms_ref,
    resid_ref,
    out_ref,
    pair_in,
    staged,
    landed,
    total,
    pair_send,
    pair_recv,
    send_sem,
    recv_sem,
):
    at = Place(chips)
    far = at.far
    meet(at.partners())
    pairs = []
    for row in (at.across_row, at.first_row, at.second_row, at.own_row):
        for step in list(range(1, far)) + [0]:
            chip = at.chip_of(step, row)
            pair = remote(
                terms_ref.at[chip * 2 + 1 - at.core],
                pair_in.at[chip],
                pair_send.at[chip],
                pair_recv.at[chip],
                at.sibling,
            )
            pair.start()
            pairs.append(pair)
    sends, waiting = {}, []

    def own_sum(step, row, slots):
        chip = at.chip_of(step, row)
        remote(
            terms_ref.at[chip * 2 + 1 - at.core],
            pair_in.at[chip],
            pair_send.at[chip],
            pair_recv.at[chip],
            at.sibling,
        ).wait_recv()
        value = terms_ref[chip * 2 + at.core].astype(jnp.float32)
        value = value + pair_in[chip].astype(jnp.float32)
        for slot in slots:
            sends[slot].wait_recv()
            value = value + landed[slot].astype(jnp.float32)
        return value

    def flush():
        while waiting:
            waiting.pop().start()

    def send(slot, value, device):
        staged[slot] = value.astype(staged.dtype)
        sends[slot] = remote(
            staged.at[slot], landed.at[slot], send_sem.at[slot], recv_sem.at[slot], device
        )
        flush()
        waiting.append(sends[slot])

    steps = list(range(1, far)) + [0]
    for step in steps:
        send(far + step, own_sum(step, at.across_row, []), at.second)
    for step in steps:
        send(step, own_sum(step, at.second_row, []), at.second)
    flush()
    for step in steps:
        send(2 * far + step, own_sum(step, at.first_row, [far + step]), at.first)
    flush()
    for step in steps[:-1]:
        value = own_sum(step, at.own_row, [step, 2 * far + step])
        send(3 * far + step - 1, value, at.block(step, at.own_row))
    flush()
    total[...] = resid_ref[...].astype(jnp.float32) + own_sum(0, at.own_row, [0, 2 * far])
    for step in steps[:-1]:
        sends[3 * far + step - 1].wait_recv()
        total[...] += landed[3 * far + step - 1].astype(jnp.float32)
    out_ref[...] = total[...].astype(out_ref.dtype)
    for copy in sends.values():
        copy.wait_send()
    for pair in pairs:
        pair.wait_send()


def scatter_rows(terms, resid):
    n, rows, width = terms.shape
    chips = n // 2
    return pl.pallas_call(
        functools.partial(scatter_kernel, chips),
        out_shape=jax.ShapeDtypeStruct(resid.shape, resid.dtype),
        in_specs=[pl.BlockSpec(memory_space=pltpu.VMEM)] * 2,
        out_specs=pl.BlockSpec(memory_space=pltpu.VMEM),
        scratch_shapes=[
            pltpu.VMEM((chips, rows, width), terms.dtype),
            pltpu.VMEM((chips - 1, rows, width), terms.dtype),
            pltpu.VMEM((chips - 1, rows, width), terms.dtype),
            pltpu.VMEM((rows, width), jnp.float32),
            pltpu.SemaphoreType.DMA((chips,)),
            pltpu.SemaphoreType.DMA((chips,)),
            pltpu.SemaphoreType.DMA((chips - 1,)),
            pltpu.SemaphoreType.DMA((chips - 1,)),
        ],
        compiler_params=pltpu.CompilerParams(collective_id=1, has_side_effects=True),
        name="scatter_rows",
    )(terms, resid)


def branch_kernel(
    stride, width, steps, x_ref, dg_ref, du_ref, dd_ref, eg_ref, eu_ref, ed_ref, out_ref, total
):
    me = lax.axis_index("ep")
    step = pl.program_id(1)
    x = x_ref[:, :width]
    scales = x_ref[:, width:].astype(jnp.float32)
    column = lax.broadcasted_iota(jnp.int32, scales.shape, 1)

    def scale_of(owner):
        held = (column == owner) | (column == owner + stride) | (column == owner + 2 * stride)
        return jnp.sum(jnp.where(held, scales, 0.0), axis=1, keepdims=True)

    def branch(w_gate, w_up, w_down, scale):
        gate_part = jnp.dot(x, w_gate, preferred_element_type=jnp.float32)
        up_part = jnp.dot(x, w_up, preferred_element_type=jnp.float32)
        hidden = (scale * jax.nn.silu(gate_part) * up_part).astype(jnp.bfloat16)
        return jnp.dot(hidden, w_down, preferred_element_type=jnp.float32)

    terms = branch(dg_ref[...], du_ref[...], dd_ref[...], scale_of(stride - 1))
    terms = terms + branch(eg_ref[0], eu_ref[0], ed_ref[0], scale_of(me))
    if steps > 1:

        @pl.when(step == 0)
        def _():
            total[...] = terms

        @pl.when(step > 0)
        def _():
            total[...] += terms

        @pl.when(step == steps - 1)
        def _():
            out_ref[...] = total[...].astype(out_ref.dtype)
    else:
        out_ref[...] = terms.astype(out_ref.dtype)


def branch_terms(gathered, width, stride, dense, expert):
    count = gathered.shape[0]
    dense_units, expert_units = dense[0].shape[1], expert[0].shape[2]
    steps = 2 if dense_units % 256 == 0 and expert_units % 256 == 0 else 1
    tile = 512 if count % 512 == 0 else count
    dense_tile, expert_tile = dense_units // steps, expert_units // steps
    dense_in = pl.BlockSpec((width, dense_tile), lambda r, j: (0, j))
    expert_in = pl.BlockSpec((1, width, expert_tile), lambda r, j: (0, 0, j))
    return pl.pallas_call(
        functools.partial(branch_kernel, stride, width, steps),
        grid=(count // tile, steps),
        out_shape=jax.ShapeDtypeStruct((count, width), jnp.bfloat16),
        in_specs=[
            pl.BlockSpec((tile, gathered.shape[1]), lambda r, j: (r, 0)),
            dense_in,
            dense_in,
            pl.BlockSpec((dense_tile, width), lambda r, j: (j, 0)),
            expert_in,
            expert_in,
            pl.BlockSpec((1, expert_tile, width), lambda r, j: (0, j, 0)),
        ],
        out_specs=pl.BlockSpec((tile, width), lambda r, j: (r, 0)),
        scratch_shapes=[pltpu.VMEM((tile, width), jnp.float32)],
        compiler_params=pltpu.CompilerParams(vmem_limit_bytes=50 * 1024 * 1024),
        name="branch_terms",
    )(gathered, *dense, *expert)


def in_pieces(values):
    high = lax.reduce_precision(values, 8, 7)
    middle = lax.reduce_precision(values - high, 8, 7)
    return jnp.concatenate([high, middle, values - high - middle], axis=1).astype(jnp.bfloat16)


def on_device(
    n,
    tokens,
    state,
    norm_mix,
    w_drive,
    lam_real,
    lam_imag,
    log_step,
    b_real,
    b_imag,
    readout_real,
    readout_imaginary,
    d_skip,
    w_value,
    w_glugate,
    w_output,
    norm_ffn,
    w_group,
    w_expert,
    route_ids,
    expert_gate,
    expert_up,
    expert_down,
    dense_vector,
    dense_gate,
    dense_up,
    dense_down,
):
    resid, new_state = state_mixer(
        tokens,
        state,
        norm_mix,
        w_drive,
        lam_real,
        lam_imag,
        log_step,
        b_real,
        b_imag,
        readout_real,
        readout_imaginary,
        d_skip,
        w_value,
        w_glugate,
        w_output,
    )
    normed = rms_scale(resid, norm_ffn)
    expert_count = w_expert.shape[1]
    rows, width = normed.shape
    gates = route_gates(normed, w_group, w_expert, route_ids)
    branch_gate = jax.nn.sigmoid(
        jnp.dot(normed.astype(jnp.float32), dense_vector, precision=HIGH_PRECISION)
    )
    scales = in_pieces(jnp.concatenate([gates, branch_gate[:, None]], axis=1))
    scales = jnp.pad(scales, ((0, 0), (0, -scales.shape[1] % 128)))
    gathered = gather_rows(jnp.concatenate([normed, scales], axis=1), n)
    gathered = gathered.reshape(n * rows, -1)
    terms = branch_terms(
        gathered,
        width,
        expert_count + 1,
        (dense_gate, dense_up, dense_down),
        (expert_gate, expert_up, expert_down),
    )
    layer_out = scatter_rows(terms.reshape(n, rows, width), resid)
    return (layer_out, new_state)


def solution(mesh):
    placed = (
        P("ep", None),
        P(None, "ep", None),
        P(),
        P(),
        P(),
        P(),
        P(),
        P(),
        P(),
        P(),
        P(),
        P(),
        P(),
        P(),
        P(),
        P(),
        P(),
        P(),
        P("ep", None),
        P("ep", None, None),
        P("ep", None, None),
        P("ep", None, None),
        P(),
        P(None, "ep"),
        P(None, "ep"),
        P("ep", None),
    )
    return jax.shard_map(
        functools.partial(on_device, mesh.shape["ep"]),
        mesh=mesh,
        in_specs=placed,
        out_specs=(P("ep", None), P(None, "ep", None)),
        check_vma=False,
    )
```
